32 devices in a mesh: grp: 2 (over y), sp: 4 (over z), tp: 4 (over x, core).
Axes of the slice: x: 2, y: 2, z: 4, core: 2. Of those that a mesh axis runs over, the one named last changes fastest.
Arguments:
- queries: bfloat16 [4096, 1024], P(('grp', 'sp'), 'tp'), parts along dimension 0, may hold values from -120 to 120
- keys: bfloat16 [4096, 256], P(('grp', 'sp')), parts along dimension 0, may hold values from -6 to 6
- values: bfloat16 [4096, 256], P(('grp', 'sp')), parts along dimension 0, may hold values from -6 to 6
- sink: float32 [8], P('tp'), may hold values from 1 to 5
- resid: bfloat16 [4096, 2048], P(('grp', 'sp')), parts along dimension 0, may hold values from -100 to 100
- out_proj: bfloat16 [1024, 2048], P(None, 'tp'), may hold values from -1.5 to 1.5
- norm_gain: float32 [2048], replicated, may hold values from 0.1 to 1.9
- w_gate: bfloat16 [2048, 6144], P('sp', 'tp'), may hold values from -0.125 to 0.125
- w_up: bfloat16 [2048, 6144], P('sp', 'tp'), may hold values from -0.125 to 0.125
- conv_w: float32 [3, 6144], P(None, 'tp'), may hold values from -3 to 3
- conv_b: float32 [6144], P('tp'), may hold values from -3 to 3
- w_down: bfloat16 [6144, 2048], P('tp', 'sp'), may hold values from -0.21875 to 0.21875
Outputs:
- layer_out: bfloat16 [4096, 2048], P(('grp', 'sp'), 'tp'), parts along dimension 0
The draws below stay inside these ranges and needn't reach their ends.
There are 2 independent parts, one for each index of `grp`. The reference program is written for one: setup_inputs(seed, part) draws one part's arguments, and reference() takes and returns one part's arrays. A program takes and returns all parts, laid end to end along the dimension named above; an argument that names none is the same for every part. Nothing has to cross between parts.
All inputs are finite; a program needn't handle non-finite values.
Results may differ from the reference program's by a relative error of at most 0.015.
Values may be sent and summed in bfloat16 or wider, within the bound.
No kernel may reach another device: no remote copies, remote signals or barrier semaphores. Data moves between devices by JAX's collectives and lax.ppermute only.
A program may use at most 64 MiB of HBM per device.

```python
import jax
import jax.numpy as jnp
from jax import lax

D = 2048
FF = 6144
H = 8
KVH = 2
HD = 128
WINDOW = 128
CONV = 3
TOK_DEV = 512
SEQ = 2048


def joint_qk(key):
    base = jax.random.fold_in(key, 11)
    key_q, key_k = jax.random.split(base)
    q_vals = jnp.clip(jax.random.normal(key_q, (SEQ, H, HD), jnp.float32), -6.0, 6.0)
    k_vals = jnp.clip(jax.random.normal(key_k, (SEQ, KVH, HD), jnp.float32), -6.0, 6.0)
    return (q_vals.reshape(SEQ, H * HD), k_vals.reshape(SEQ, KVH * HD))


def draw_queries(key, part):
    return joint_qk(key)[0].astype(jnp.bfloat16)


def draw_keys(key, part):
    return joint_qk(key)[1].astype(jnp.bfloat16)


def draw_resid(key, part):
    base = jax.random.fold_in(key, 23)
    key_n, key_r, key_c = jax.random.split(base, 3)
    trend = 0.5 + jnp.arange(D, dtype=jnp.float32) / D
    columns = jnp.exp(jax.random.uniform(key_c, (D,), jnp.float32, -0.7, 0.7)) * trend
    noise = jnp.clip(jax.random.normal(key_n, (SEQ, D), jnp.float32), -6.0, 6.0)
    rows = jnp.exp(jax.random.uniform(key_r, (SEQ, 1), jnp.float32, -0.69, 1.6))
    return jnp.clip(noise * rows * columns[None, :], -100.0, 100.0).astype(jnp.bfloat16)


def spiked(array, key, source, target, blocks, factor):
    def block_of(dim):
        return (jnp.arange(array.shape[dim]) // (array.shape[dim] // blocks)).reshape((-1,) + (1,) * (array.ndim - 1 - dim))

    first = jax.random.permutation(key, blocks)[block_of(target)]
    other_side = (block_of(target) + blocks // 2) % blocks
    return jnp.where((block_of(source) == first) | (block_of(source) == other_side), factor * array, array)


def steps_of(own_key, dims, cuts, least, high):
    loudness, own = 1.0, jax.random.fold_in(own_key, 6)
    for dim, parts in cuts:
        draws = jnp.exp(jax.random.uniform(jax.random.fold_in(own, dim), (parts,), jnp.float32, least / len(cuts), high / len(cuts)))
        loudness = loudness * jnp.repeat(draws, dims[dim] // parts).reshape([-1 if axis == dim else 1 for axis in range(len(dims))])
    return loudness


def gaussian(key, shape, scale, most, cuts=(), kind=jnp.bfloat16):
    drawn = scale * jax.random.normal(key, shape, jnp.float32)
    if cuts:
        drawn = drawn * steps_of(key, shape, cuts, -0.22, 0.18)
    return jnp.clip(drawn, -most, most).astype(kind)


def noise_with(own_key, extent, scale, reach, cuts, heavy, held_as=jnp.bfloat16):
    drawn = scale * jax.random.normal(own_key, extent, jnp.float32)
    if cuts:
        drawn = drawn * steps_of(own_key, extent, cuts, -0.22, 0.18)
    return jnp.clip(spiked(drawn, jax.random.fold_in(own_key, 3), *heavy), -reach, reach).astype(held_as)


def setup_inputs(seed: int = 0, part: int = 0) -> dict:
    key_list = jax.random.split(jax.random.key(seed), 13)
    own_keys = jax.random.split(jax.random.fold_in(key_list[12], part), 13)
    return {
        "queries": draw_queries(jax.random.fold_in(jax.random.fold_in(key_list[12], part), 71), part),
        "keys": draw_keys(jax.random.fold_in(jax.random.fold_in(key_list[12], part), 71), part),
        "values": gaussian(own_keys[2], (SEQ, KVH * HD), 1.0, 6.0, ((0, 4),)),
        "sink": jnp.clip(1.0 + 4.0 * jax.random.uniform(key_list[3], (H,), jnp.float32) ** steps_of(key_list[3], (H,), ((0, 4),), -0.2, 0.2), 1.0, 5.0),
        "resid": draw_resid(jax.random.fold_in(jax.random.fold_in(key_list[12], part), 71), part),
        "out_proj": gaussian(key_list[5], (H * HD, D), (H * HD // 64) ** -0.5, 1.5, ((1, 4),)),
        "norm_gain": jnp.clip(1.0 + 0.18 * jax.random.normal(key_list[6], (D,), jnp.float32), 0.1, 1.9),
        "w_gate": gaussian(key_list[7], (D, FF), D ** -0.5, 0.125, ((0, 4), (1, 4))),
        "w_up": gaussian(key_list[8], (D, FF), D ** -0.5, 0.125, ((0, 4), (1, 4))),
        "conv_w": gaussian(key_list[9], (CONV, FF), 0.6, 3.0, ((1, 4),), jnp.float32),
        "conv_b": gaussian(key_list[10], (FF,), 0.5, 3.0, ((0, 4),), jnp.float32),
        "w_down": noise_with(key_list[11], (FF, D), (FF // 4) ** -0.5, 0.21875, ((0, 4), (1, 4)), (0, 1, 4, 2.0)),
    }


def reference(queries, keys, values, sink, resid, out_proj, norm_gain, w_gate, w_up, conv_w, conv_b, w_down):
    group = H // KVH
    scale = HD ** (-0.5)
    span = TOK_DEV + 2 * WINDOW
    q_heads = queries.reshape(SEQ, H, HD)
    k_pad = jnp.pad(keys.reshape(SEQ, KVH, HD), ((WINDOW, WINDOW), (0, 0), (0, 0)))
    v_pad = jnp.pad(values.reshape(SEQ, KVH, HD), ((WINDOW, WINDOW), (0, 0), (0, 0)))
    sink_grid = sink.reshape(KVH, group)[:, :, None]

    def block(index):
        start = (index * TOK_DEV).astype(jnp.int32)
        q_block = lax.dynamic_slice_in_dim(q_heads, start, TOK_DEV, 0).astype(jnp.float32)
        q_block = q_block.reshape(TOK_DEV, KVH, group, HD)
        k_block = lax.dynamic_slice_in_dim(k_pad, start, span, 0).astype(jnp.float32)
        v_block = lax.dynamic_slice_in_dim(v_pad, start, span, 0).astype(jnp.float32)
        scores = jnp.einsum('qhgd,khd->hgqk', q_block, k_block) * scale
        q_pos = start + jnp.arange(TOK_DEV, dtype=jnp.int32)[:, None]
        k_pos = start - WINDOW + jnp.arange(span, dtype=jnp.int32)[None, :]
        valid = (jnp.abs(q_pos - k_pos) <= WINDOW) & (k_pos >= 0) & (k_pos < SEQ)
        scores = jnp.where(valid, scores, jnp.float32(-1e+30))
        top = jnp.maximum(lax.optimization_barrier(jnp.max(scores, axis=-1)), sink_grid)
        expo = jnp.exp(scores - top[..., None])
        total = lax.optimization_barrier(jnp.sum(expo, axis=-1)) + jnp.exp(sink_grid - top)
        weights = (expo / total[..., None]).astype(jnp.bfloat16)
        out = jnp.einsum('hgqk,khd->qhgd', weights.astype(jnp.float32), v_block)
        return out.astype(jnp.bfloat16).reshape(TOK_DEV, H * HD)
    mixed = lax.map(block, jnp.arange(SEQ // TOK_DEV, dtype=jnp.int32)).reshape(SEQ, H * HD)
    summed = resid.astype(jnp.float32) + jnp.dot(mixed, out_proj, preferred_element_type=jnp.float32)
    mean = lax.optimization_barrier(jnp.mean(summed, axis=-1, keepdims=True))
    msq = lax.optimization_barrier(jnp.mean(summed * summed, axis=-1, keepdims=True))
    normed = ((summed - mean) * lax.rsqrt(msq - mean * mean + 1e-05) * norm_gain).astype(jnp.bfloat16)
    gate_pre = jnp.dot(normed, w_gate, preferred_element_type=jnp.float32).astype(jnp.bfloat16)
    up_part = jnp.dot(normed, w_up, preferred_element_type=jnp.float32).astype(jnp.bfloat16)
    padded = jnp.pad(gate_pre.astype(jnp.float32), ((1, 1), (0, 0)))
    conv = conv_b
    for tap in range(CONV):
        conv = conv + padded[tap:tap + SEQ] * conv_w[tap]
    act = (jax.nn.silu(conv) * up_part.astype(jnp.float32)).astype(jnp.bfloat16)
    ffn = jnp.dot(act, w_down, preferred_element_type=jnp.float32)
    return (normed.astype(jnp.float32) + ffn).astype(jnp.bfloat16)
```

```python
import jax
import jax.numpy as jnp
from jax import lax
from jax.sharding import PartitionSpec as P


H = 8
KVH = 2
HD = 128
WINDOW = 128
CONV = 3
HALO = 16


def xor_pairs(count, mask):
    return [(i, i ^ mask) for i in range(count)]


def steps_of(levels):
    return sorted(range(1, levels), reverse=True)


def gather_tp(block):
    count = lax.axis_size("tp")
    slots = {0: block}
    mask = count // 2
    while mask:
        for j in sorted(slots):
            slots[j ^ mask] = lax.ppermute(slots[j], "tp", xor_pairs(count, mask))
        mask //= 2
    return slots


def attend(queries, keys, values, sink):
    tokens = queries.shape[0]
    heads_here = sink.shape[0]
    levels = lax.axis_size("sp")
    group = H // KVH
    scale = HD ** (-0.5)
    kv_head = (lax.axis_index("tp") * heads_here) // group
    own_keys = lax.dynamic_slice_in_dim(keys, kv_head * HD, HD, 1)
    own_values = lax.dynamic_slice_in_dim(values, kv_head * HD, HD, 1)
    both = jnp.stack([own_keys, own_values])
    up = [(i, i + 1) for i in range(levels - 1)]
    down = [(i + 1, i) for i in range(levels - 1)]
    before = lax.ppermute(both[:, tokens - WINDOW :], "sp", up)
    after = lax.ppermute(both[:, :WINDOW], "sp", down)
    extended = jnp.concatenate([before, both, after], axis=1)
    span = tokens + 2 * WINDOW
    q_heads = queries.reshape(tokens, heads_here, HD)
    scores = (
        jnp.einsum("qhd,kd->hqk", q_heads, extended[0], preferred_element_type=jnp.float32) * scale
    )
    offset = lax.axis_index("sp") * tokens
    q_pos = offset + jnp.arange(tokens, dtype=jnp.int32)[:, None]
    k_pos = offset - WINDOW + jnp.arange(span, dtype=jnp.int32)[None, :]
    valid = (jnp.abs(q_pos - k_pos) <= WINDOW) & (k_pos >= 0) & (k_pos < tokens * levels)
    scores = jnp.where(valid[None], scores, jnp.float32(-1e30))
    sink_col = sink[:, None]
    top = jnp.maximum(jnp.max(scores, axis=-1), sink_col)
    expo = jnp.exp(scores - top[..., None])
    total = jnp.sum(expo, axis=-1) + jnp.exp(sink_col - top)
    weights = (expo / total[..., None]).astype(jnp.bfloat16)
    mixed = jnp.einsum("hqk,kd->qhd", weights, extended[1], preferred_element_type=jnp.float32)
    return mixed.astype(jnp.bfloat16).reshape(tokens, heads_here * HD)


def layer(
    queries, keys, values, sink, resid, out_proj, norm_gain, w_gate, w_up, conv_w, conv_b, w_down
):
    tokens = queries.shape[0]
    width = resid.shape[1]
    levels = lax.axis_size("sp")
    count = lax.axis_size("tp")
    level = lax.axis_index("sp")
    tp = lax.axis_index("tp")
    part = lax.axis_index("grp")
    odd = level & 1
    cols = width // count
    rows_lv = width // levels
    hidden = w_gate.shape[1]
    half = hidden // 2

    def gu_piece(dest_odd, share):
        rows = rows_lv // 2
        return jnp.concatenate(
            [
                lax.dynamic_slice(w, (share * rows, dest_odd * half), (rows, half))
                for w in (w_gate, w_up)
            ],
            axis=1,
        )

    def d_piece(dest_odd, share):
        rows = half // 2
        return lax.dynamic_slice(w_down, (dest_odd * half + share * rows, 0), (rows, rows_lv))

    swap = [(0, 1), (1, 0)]
    gu_full = jnp.zeros((width, 2 * half), w_gate.dtype)
    d_full = jnp.zeros((half, width), w_down.dtype)

    def put_gu(full, piece, source, share):
        return lax.dynamic_update_slice(
            full, piece, (source * rows_lv + share * (rows_lv // 2), 0)
        )

    def put_d(full, piece, source, share):
        start = source * rows_lv
        slot = (start // cols) ^ tp
        place = (slot >> 1) + (slot & 1) * (count // 2)
        return lax.dynamic_update_slice(
            full, piece, (share * (half // 2), place * cols + start % cols)
        )

    for share in range(2):
        gu_full = put_gu(gu_full, gu_piece(odd, share), level, share)
        d_full = put_d(d_full, d_piece(odd, share), level, share)
    for mask in steps_of(levels):
        got = lax.ppermute(gu_piece(odd ^ (mask & 1), part), "sp", xor_pairs(levels, mask))
        other = lax.ppermute(got, "grp", swap)
        gu_full = put_gu(gu_full, got, level ^ mask, part)
        gu_full = put_gu(gu_full, other, level ^ mask, 1 - part)
    for mask in steps_of(levels):
        got = lax.ppermute(d_piece(odd ^ (mask & 1), part), "sp", xor_pairs(levels, mask))
        other = lax.ppermute(got, "grp", swap)
        d_full = put_d(d_full, got, level ^ mask, part)
        d_full = put_d(d_full, other, level ^ mask, 1 - part)

    mixed = attend(queries, keys, values, sink)
    head_cols = mixed.shape[1]
    all_heads = jnp.zeros((tokens, count * head_cols), mixed.dtype)
    for j, block in gather_tp(mixed).items():
        all_heads = lax.dynamic_update_slice(all_heads, block, (0, (tp ^ j) * head_cols))
    resid_own = lax.dynamic_slice_in_dim(resid, tp * cols, cols, 1)
    gain_own = lax.dynamic_slice_in_dim(norm_gain, tp * cols, cols, 0)
    summed = resid_own.astype(jnp.float32) + jnp.dot(
        all_heads, out_proj, preferred_element_type=jnp.float32
    )
    sums = jnp.stack([jnp.sum(summed, axis=-1), jnp.sum(summed * summed, axis=-1)])
    totals = sums
    for j in range(1, count):
        totals = totals + lax.ppermute(sums, "tp", xor_pairs(count, j))
    mean = (totals[0] / width)[:, None]
    msq = (totals[1] / width)[:, None]
    normed = ((summed - mean) * lax.rsqrt(msq - mean * mean + 1e-05) * gain_own).astype(
        jnp.bfloat16
    )

    outer = jnp.where(odd == 1, normed[tokens - HALO :], normed[:HALO])
    near = [(i, i + 1 if i & 1 else i - 1) for i in range(levels)]
    far = [(i, i + 2 if i & 1 else i - 2) for i in range(levels)]
    near = [(a, b) for a, b in near if 0 <= b < levels]
    far = [(a, b) for a, b in far if 0 <= b < levels]
    rows = 2 * tokens + 2 * HALO
    last = rows - HALO
    mate = lax.ppermute(normed, "sp", xor_pairs(levels, 1))
    edge_a = lax.ppermute(outer, "sp", near)
    edge_b = lax.ppermute(outer, "sp", far)
    pair = jnp.zeros((rows, cols), normed.dtype)
    pair = lax.dynamic_update_slice(pair, normed, (HALO + odd * tokens, 0))
    pair = lax.dynamic_update_slice(pair, mate, (HALO + (1 - odd) * tokens, 0))
    pair = lax.dynamic_update_slice(pair, edge_a, (odd * last, 0))
    pair = lax.dynamic_update_slice(pair, edge_b, ((1 - odd) * last, 0))
    normed_all = jnp.zeros((rows, width), normed.dtype)
    for j, block in gather_tp(pair).items():
        normed_all = lax.dynamic_update_slice(normed_all, block, (0, (tp ^ j) * cols))

    both = jnp.dot(normed_all, gu_full, preferred_element_type=jnp.float32).astype(jnp.bfloat16)
    taps = lax.dynamic_slice_in_dim(conv_w, odd * half, half, 1)
    conv = lax.dynamic_slice_in_dim(conv_b, odd * half, half, 0)
    first = HALO - CONV // 2
    for tap in range(CONV):
        gate = both[first + tap : first + tap + 2 * tokens, :half]
        conv = conv + gate.astype(jnp.float32) * taps[tap]
    up_part = both[HALO : HALO + 2 * tokens, half:]
    act = (jax.nn.silu(conv) * up_part.astype(jnp.float32)).astype(jnp.bfloat16)
    mine = width // 2
    away = jnp.dot(act, d_full[:, mine:], preferred_element_type=jnp.float32).astype(jnp.bfloat16)
    came = lax.ppermute(away, "tp", xor_pairs(count, 1))
    here = jnp.dot(act, d_full[:, :mine], preferred_element_type=jnp.float32)
    here = here + came.astype(jnp.float32)

    def block_of(step, slot):
        start = (odd ^ step) * tokens
        return lax.dynamic_slice(here, (start, slot * cols), (tokens, cols))

    ffn = block_of(0, 0)
    for step in range(2):
        for slot in range(count // 2):
            if step or slot:
                pairs = [
                    (i * count + j, (i ^ step) * count + (j ^ (2 * slot)))
                    for i in range(levels)
                    for j in range(count)
                ]
                ffn = ffn + lax.ppermute(
                    block_of(step, slot).astype(jnp.bfloat16), ("sp", "tp"), pairs
                ).astype(jnp.float32)
    return (normed.astype(jnp.float32) + ffn).astype(jnp.bfloat16)


def solution(mesh):
    return jax.shard_map(
        layer,
        mesh=mesh,
        in_specs=(
            P(("grp", "sp"), "tp"),
            P(("grp", "sp"), None),
            P(("grp", "sp"), None),
            P("tp"),
            P(("grp", "sp"), None),
            P(None, "tp"),
            P(),
            P("sp", "tp"),
            P("sp", "tp"),
            P(None, "tp"),
            P("tp"),
            P("tp", "sp"),
        ),
        out_specs=P(("grp", "sp"), "tp"),
        check_vma=False,
    )
```

```python
import functools

import jax
import jax.numpy as jnp
from jax import lax
from jax.experimental import pallas as pl
from jax.experimental.pallas import tpu as pltpu
from jax.sharding import PartitionSpec as P


H = 8
KVH = 2
HD = 128
WINDOW = 128
CONV = 3
HALO = 16


SWAP = [(0, 1), (1, 0)]


def send(cells, axis, pairs):
    return lax.ppermute(cells, axis, pairs)


def xor_pairs(count, mask):
    return [(i, i ^ mask) for i in range(count)]


def attend(queries, keys, values, sink):
    tokens = queries.shape[0]
    heads_here = sink.shape[0]
    levels = lax.axis_size("sp")
    group = H // KVH
    scale = HD ** (-0.5)
    kv_head = (lax.axis_index("tp") * heads_here) // group
    own_keys = lax.dynamic_slice_in_dim(keys, kv_head * HD, HD, 1)
    own_values = lax.dynamic_slice_in_dim(values, kv_head * HD, HD, 1)
    both = jnp.stack([own_keys, own_values])
    up = [(i, i + 1) for i in range(levels - 1)]
    down = [(i + 1, i) for i in range(levels - 1)]
    before = send(both[:, tokens - WINDOW :], "sp", up)
    after = send(both[:, :WINDOW], "sp", down)
    extended = jnp.concatenate([before, both, after], axis=1)
    span = tokens + 2 * WINDOW
    q_heads = queries.reshape(tokens, heads_here, HD)
    scores = (
        jnp.einsum("qhd,kd->hqk", q_heads, extended[0], preferred_element_type=jnp.float32) * scale
    )
    offset = lax.axis_index("sp") * tokens
    q_pos = offset + jnp.arange(tokens, dtype=jnp.int32)[:, None]
    k_pos = offset - WINDOW + jnp.arange(span, dtype=jnp.int32)[None, :]
    valid = (jnp.abs(q_pos - k_pos) <= WINDOW) & (k_pos >= 0) & (k_pos < tokens * levels)
    scores = jnp.where(valid[None], scores, jnp.float32(-1e30))
    sink_col = sink[:, None]
    top = jnp.maximum(jnp.max(scores, axis=-1), sink_col)
    expo = jnp.exp(scores - top[..., None])
    total = jnp.sum(expo, axis=-1) + jnp.exp(sink_col - top)
    weights = (expo / total[..., None]).astype(jnp.bfloat16)
    mixed = jnp.einsum("hqk,kd->qhd", weights, extended[1], preferred_element_type=jnp.float32)
    return mixed.astype(jnp.bfloat16).reshape(tokens, heads_here * HD)


def gather_tp(block):
    count = lax.axis_size("tp")
    slots = {0: block}
    mask = count // 2
    while mask:
        for j in sorted(slots):
            slots[j ^ mask] = send(slots[j], "tp", xor_pairs(count, mask))
        mask //= 2
    return slots


def side_by_side(slots):
    count, tp = lax.axis_size("tp"), lax.axis_index("tp")
    rows, cols = slots[0].shape
    full = jnp.zeros((rows, count * cols), slots[0].dtype)
    for j, block in slots.items():
        full = lax.dynamic_update_slice(full, block, (0, (tp ^ j) * cols))
    return full


def normalize(queries, keys, values, sink, resid, out_proj, norm_gain):
    _, width = resid.shape
    count, tp = lax.axis_size("tp"), lax.axis_index("tp")
    cols = width // count
    mixed = attend(queries, keys, values, sink)
    all_heads = side_by_side(gather_tp(mixed))
    resid_own = lax.dynamic_slice_in_dim(resid, tp * cols, cols, 1)
    gain_own = lax.dynamic_slice_in_dim(norm_gain, tp * cols, cols, 0)
    summed = resid_own.astype(jnp.float32) + jnp.dot(
        all_heads, out_proj, preferred_element_type=jnp.float32
    )
    sums = jnp.stack([jnp.sum(summed, axis=-1), jnp.sum(summed * summed, axis=-1)])
    totals = sums
    for j in range(1, count):
        totals = totals + send(sums, "tp", xor_pairs(count, j))
    mean = (totals[0] / width)[:, None]
    msq = (totals[1] / width)[:, None]
    return ((summed - mean) * lax.rsqrt(msq - mean * mean + 1e-05) * gain_own).astype(
        jnp.bfloat16
    )


def shards(
    queries, keys, values, sink, resid, out_proj, norm_gain, w_gate, w_up, conv_w, conv_b, w_down
):
    fits = lax.axis_size("sp") == lax.axis_size("tp") == 4 and lax.axis_size("grp") == 2
    run = layer_of_four if fits else layer
    return run(
        queries, keys, values, sink, resid, out_proj, norm_gain,
        w_gate, w_up, conv_w, conv_b, w_down,
    )


def spread(full, piece_of, put):
    levels, level, part = lax.axis_size("sp"), lax.axis_index("sp"), lax.axis_index("grp")
    side = level // (levels // 2)
    for share in range(2):
        full = put(full, piece_of(side, share), level, share)
    for mask in range(1, levels):
        cells = piece_of((level ^ mask) // (levels // 2), part)
        got = send(cells, "sp", xor_pairs(levels, mask))
        other = send(got, "grp", SWAP)
        full = put(full, got, level ^ mask, part)
        full = put(full, other, level ^ mask, 1 - part)
    return full


def layer(
    queries, keys, values, sink, resid, out_proj, norm_gain, w_gate, w_up, conv_w, conv_b, w_down
):
    tokens = queries.shape[0]
    width = resid.shape[1]
    levels = lax.axis_size("sp")
    count = lax.axis_size("tp")
    level = lax.axis_index("sp")
    tp = lax.axis_index("tp")
    side = level // (levels // 2)
    cols = width // count
    rows_lv = width // levels
    half = w_gate.shape[1] // 2
    quarter = half // 2

    def gu_piece(of_side, share):
        rows = rows_lv // 2
        return jnp.concatenate(
            [
                lax.dynamic_slice(w, (share * rows, of_side * half), (rows, half))
                for w in (w_gate, w_up)
            ],
            axis=1,
        )

    def put_gu(full, piece, origin, share):
        return lax.dynamic_update_slice(full, piece[None, None], (origin, share, 0, 0))

    def d_piece(of_side, share):
        return lax.dynamic_slice(w_down, (of_side * half + share * quarter, 0), (quarter, rows_lv))

    per = levels // count

    def put_d(full, piece, origin, share):
        slot = (origin // per) ^ tp
        place = (slot >> 1) + (slot & 1) * (count // 2)
        return lax.dynamic_update_slice(
            full, piece[None, None], (place, share, 0, (origin % per) * rows_lv)
        )

    gu_full = jnp.zeros((levels, 2, rows_lv // 2, 2 * half), w_gate.dtype)
    gu_full = spread(gu_full, gu_piece, put_gu)
    gu_full = gu_full.reshape(width, 2 * half)
    d_full = jnp.zeros((count, 2, quarter, cols), w_down.dtype)
    d_full = spread(d_full, d_piece, put_d)
    d_full = d_full.reshape(count, half, cols)

    normed = normalize(queries, keys, values, sink, resid, out_proj, norm_gain)

    mate = levels // 2
    up = [(i, i + 1) for i in range(levels - 1)]
    down = [(i + 1, i) for i in range(levels - 1)]
    tail, head = normed[tokens - HALO :], normed[:HALO]
    other = send(normed, "sp", xor_pairs(levels, mate))
    own_before = send(tail, "sp", up)
    own_after = send(head, "sp", down)
    other_before = send(tail, "sp", [(a, b ^ mate) for a, b in up])
    other_after = send(head, "sp", [(a, b ^ mate) for a, b in down])
    pack = jnp.concatenate([other_before, other, other_after, own_before, own_after])
    normed_own = side_by_side(gather_tp(normed))
    normed_pack = side_by_side(gather_tp(pack))

    taps = lax.dynamic_slice_in_dim(conv_w, side * half, half, 1)
    bias = lax.dynamic_slice_in_dim(conv_b, side * half, half, 0)
    own_gu = jnp.dot(normed_own, gu_full, preferred_element_type=jnp.float32).astype(jnp.bfloat16)
    pack_gu = jnp.dot(normed_pack, gu_full, preferred_element_type=jnp.float32).astype(
        jnp.bfloat16
    )
    around = tokens + 2 * HALO

    def activate(gate, up_part):
        first = HALO - CONV // 2
        conv = bias
        for tap in range(CONV):
            conv = conv + gate[first + tap : first + tap + tokens].astype(jnp.float32) * taps[tap]
        return (jax.nn.silu(conv) * up_part.astype(jnp.float32)).astype(jnp.bfloat16)

    own_gate = jnp.concatenate(
        [pack_gu[around : around + HALO, :half], own_gu[:, :half], pack_gu[around + HALO :, :half]]
    )
    act_own = activate(own_gate, own_gu[:, half:])
    act_other = activate(pack_gu[:around, :half], pack_gu[HALO : HALO + tokens, half:])

    def partial(act, place):
        return jnp.dot(act, d_full[place], preferred_element_type=jnp.float32)

    def over_tp(act):
        pairs_here = count // 2
        away = [partial(act, pairs_here + i).astype(jnp.bfloat16) for i in range(pairs_here)]
        came = send(jnp.stack(away), "tp", xor_pairs(count, 1))
        here = [partial(act, i) + came[i].astype(jnp.float32) for i in range(pairs_here)]
        total = here[0]
        for i in range(1, pairs_here):
            block = send(here[i].astype(jnp.bfloat16), "tp", xor_pairs(count, 2 * i))
            total = total + block.astype(jnp.float32)
        return total

    sum_other = over_tp(act_other).astype(jnp.bfloat16)
    back = send(sum_other, "sp", xor_pairs(levels, mate))
    sum_own = over_tp(act_own)
    return (normed.astype(jnp.float32) + sum_own + back.astype(jnp.float32)).astype(jnp.bfloat16)


def gate_up_kernel(
    x0, x1, x2, x3, o0, o1, o2, o3, e0, e1, e2, e3, w_gate, w_up, z1, y1, z2, y2, z3, y3, taps, bias,
    out, xs, es, ws, gate, sems,
):
    tokens, cols = x0.shape
    half = taps.shape[1]
    rows = z1.shape[0]
    level, tp, part = lax.axis_index("sp"), lax.axis_index("tp"), lax.axis_index("grp")
    odd = level & 1
    copies = []

    def copy(source, target):
        item = pltpu.make_async_copy(source, target, sems.at[len(copies)])
        item.start()
        copies.append(item)

    copy(w_gate.at[:, pl.ds(pl.multiple_of(odd * half, half), half)], ws.at[0:cols, 0:half])
    copy(w_up.at[:, pl.ds(pl.multiple_of(odd * half, half), half)], ws.at[0:cols, half : 2 * half])
    own_rows = pl.ds(pl.multiple_of(odd * tokens, tokens), tokens)
    other_rows = pl.ds(pl.multiple_of((1 - odd) * tokens, tokens), tokens)
    columns = ((x0, o0, e0), (x1, o1, e1), (x2, o2, e2), (x3, o3, e3))
    for j, (mine, other, edge) in enumerate(columns):
        lanes = pl.ds(pl.multiple_of((tp ^ j ^ level) * cols, cols), cols)
        copy(mine, xs.at[own_rows, lanes])
        copy(other, xs.at[other_rows, lanes])
        copy(edge, es.at[:, lanes])
    for mask, (z, y) in enumerate(((z1, y1), (z2, y2), (z3, y3)), 1):
        base = mask * cols
        copy(z, ws.at[pl.ds(pl.multiple_of(base + part * rows, rows), rows), :])
        copy(y, ws.at[pl.ds(pl.multiple_of(base + (1 - part) * rows, rows), rows), :])
    for item in copies:
        item.wait()

    step = 256
    around = jnp.dot(es[...], ws[:, :half], preferred_element_type=jnp.float32)
    around = around.astype(jnp.bfloat16).astype(jnp.float32)
    even = odd == 0
    gate[7:8, :] = jnp.where(even, around[HALO - 1 : HALO], around[2 * HALO - 1 : 2 * HALO])
    gate[8 + 2 * tokens : 9 + 2 * tokens, :] = jnp.where(even, around[HALO : HALO + 1], around[0:1])

    def gates(i, carry):
        cells = xs[pl.ds(pl.multiple_of(i * step, step), step), :]
        acc = jnp.dot(cells, ws[:, :half], preferred_element_type=jnp.float32)
        gate[pl.ds(pl.multiple_of(8 + i * step, 8), step), :] = acc.astype(jnp.bfloat16).astype(
            jnp.float32
        )
        return carry

    lax.fori_loop(0, 2 * tokens // step, gates, 0)
    for start in range(0, 2 * tokens, step):
        cells = xs[start : start + step, :]
        acc = jnp.dot(cells, ws[:, half:], preferred_element_type=jnp.float32)
        up_part = acc.astype(jnp.bfloat16).astype(jnp.float32)
        conv = bias[...]
        for tap in range(CONV):
            conv = conv + gate[7 + tap + start : 7 + tap + start + step, :] * taps[tap : tap + 1, :]
        silu = conv / (1.0 + jnp.exp(-conv))
        out[start : start + step, :] = (silu * up_part).astype(jnp.bfloat16)


def gate_up(own, other, edges, w_gate, w_up, pieces, taps, bias):
    tokens, cols = own[0].shape
    half = taps.shape[1]
    width = 4 * cols
    near, far = pl.BlockSpec(memory_space=pl.ANY), pl.BlockSpec(memory_space=pltpu.VMEM)
    return pl.pallas_call(
        gate_up_kernel,
        out_shape=jax.ShapeDtypeStruct((2 * tokens, half), jnp.bfloat16),
        in_specs=[near] * 20 + [far] * 2,
        out_specs=far,
        scratch_shapes=[
            pltpu.VMEM((2 * tokens, width), jnp.bfloat16),
            pltpu.VMEM((2 * HALO, width), jnp.bfloat16),
            pltpu.VMEM((width, 2 * half), jnp.bfloat16),
            pltpu.VMEM((2 * tokens + HALO, half), jnp.float32),
            pltpu.SemaphoreType.DMA((20,)),
        ],
        compiler_params=pltpu.CompilerParams(vmem_limit_bytes=40 * 2**20),
        name="gate_up",
    )(*own, *other, *edges, w_gate, w_up, *pieces, taps, bias)


def down_kernel(parity, act, w_down, z1, y1, z2, y2, z3, y3, out, ds, sems):
    tokens, _ = out.shape[2:]
    half = act.shape[1]
    quarter = half // 2
    level, tp, part = lax.axis_index("sp"), lax.axis_index("tp"), lax.axis_index("grp")
    odd = level & 1
    lower = pl.ds(pl.multiple_of(part * quarter, quarter), quarter)
    upper = pl.ds(pl.multiple_of((1 - part) * quarter, quarter), quarter)
    copies = []
    for mask in range(4):
        slot = level ^ mask ^ tp
        if mask == 0:
            own = w_down.at[pl.ds(pl.multiple_of(odd * half, half), half), :]
            parts = [(own, ds.at[slot])]
        else:
            z, y = ((z1, y1), (z2, y2), (z3, y3))[mask - 1]
            parts = [(z, ds.at[slot, lower, :]), (y, ds.at[slot, upper, :])]
        for source, target in parts:
            item = pltpu.make_async_copy(source, target, sems.at[len(copies)])
            item.start()
            copies.append(item)
    for item in copies:
        item.wait()
    for which in range(2):
        block = odd if which else 1 - odd
        cells = act[pl.ds(pl.multiple_of(block * tokens, tokens), tokens), :]
        for i in range(2):
            out[which, i] = jnp.dot(
                cells, ds[2 * i + parity], preferred_element_type=jnp.float32
            ).astype(out.dtype)


def down(act, w_down, pieces, parity, dtype):
    tokens, half = act.shape[0] // 2, act.shape[1]
    cols = w_down.shape[1]
    near, far = pl.BlockSpec(memory_space=pl.ANY), pl.BlockSpec(memory_space=pltpu.VMEM)
    return pl.pallas_call(
        functools.partial(down_kernel, parity),
        out_shape=jax.ShapeDtypeStruct((2, 2, tokens, cols), dtype),
        in_specs=[far] + [near] * 7,
        out_specs=far,
        scratch_shapes=[pltpu.VMEM((4, half, cols), jnp.bfloat16), pltpu.SemaphoreType.DMA((7,))],
        compiler_params=pltpu.CompilerParams(vmem_limit_bytes=24 * 2**20),
    )(act, w_down, *pieces)


def travel(piece_of):
    odd, part = lax.axis_index("sp") & 1, lax.axis_index("grp")
    pieces = []
    for mask in range(1, 4):
        z = send(piece_of(odd ^ (mask & 1), part), "sp", xor_pairs(4, mask))
        pieces += [z, send(z, "grp", SWAP)]
    return pieces


def layer_of_four(
    queries, keys, values, sink, resid, out_proj, norm_gain, w_gate, w_up, conv_w, conv_b, w_down
):
    tokens = queries.shape[0]
    odd = lax.axis_index("sp") & 1
    half = w_gate.shape[1] // 2
    quarter = half // 2

    def gu_piece(of_side, share):
        rows = w_gate.shape[0] // 2
        return jnp.concatenate(
            [
                lax.dynamic_slice(w, (share * rows, of_side * half), (rows, half))
                for w in (w_gate, w_up)
            ],
            axis=1,
        )

    def d_piece(of_side, share):
        return lax.dynamic_slice(
            w_down, (of_side * half + share * quarter, 0), (quarter, w_down.shape[1])
        )

    gu = travel(gu_piece)
    dn = travel(d_piece)
    normed = normalize(queries, keys, values, sink, resid, out_proj, norm_gain)
    mate = send(normed, "sp", xor_pairs(4, 1))
    outer = jnp.where(odd == 1, normed[tokens - HALO :], normed[:HALO])
    near = send(outer, "sp", [(1, 2), (2, 1)])
    far = send(outer, "sp", [(1, 3), (2, 0)])
    own = gather_tp(normed)
    other = gather_tp(mate)
    edges = gather_tp(jnp.concatenate([near, far]))

    taps = lax.dynamic_slice_in_dim(conv_w, odd * half, half, 1)
    bias = lax.dynamic_slice_in_dim(conv_b, odd * half, half, 0)
    act = gate_up(
        *([slots[j] for j in range(4)] for slots in (own, other, edges)),
        w_gate, w_up, gu, taps, bias[None],
    )

    away = down(act, w_down, dn, 1, jnp.bfloat16)
    came = [send(away[i], "tp", xor_pairs(4, 1)) for i in range(2)]
    here = down(act, w_down, dn, 0, jnp.float32)

    middle = tokens // 2

    def partial(which, slot, rows):
        return here[which, slot, rows] + came[which][slot, rows].astype(jnp.float32)

    def cross(cells, axis, mask):
        return send(cells.astype(jnp.bfloat16), axis, xor_pairs(4, mask)).astype(jnp.float32)

    top, low = slice(0, middle), slice(middle, tokens)
    x_other = cross(partial(0, 1, top), "tp", 2)
    z_low = cross(jnp.stack([partial(0, 0, low), partial(0, 1, low)]), "sp", 1)
    x_top = cross(partial(1, 1, top), "tp", 2)
    back = cross(partial(0, 0, top) + x_other, "sp", 1)
    x_low = cross(partial(1, 1, low) + z_low[1], "tp", 2)
    ffn = jnp.concatenate([partial(1, 0, top) + x_top + back, partial(1, 0, low) + z_low[0] + x_low])
    return (normed.astype(jnp.float32) + ffn).astype(jnp.bfloat16)


def solution(mesh):
    step = jax.shard_map(
        shards,
        mesh=mesh,
        in_specs=(
            P(("grp", "sp"), "tp"),
            P(("grp", "sp"), None),
            P(("grp", "sp"), None),
            P("tp"),
            P(("grp", "sp"), None),
            P(None, "tp"),
            P(),
            P("sp", "tp"),
            P("sp", "tp"),
            P(None, "tp"),
            P("tp"),
            P("tp", "sp"),
        ),
        out_specs=P(("grp", "sp"), "tp"),
        check_vma=False,
    )
    if not (mesh.shape["sp"] == mesh.shape["tp"] == 4 and mesh.shape["grp"] == 2):
        return step
    return step
```

```python
import jax
import jax.numpy as jnp
from jax import lax
from jax.experimental import pallas as pl
from jax.experimental.pallas import tpu as pltpu
from jax.sharding import PartitionSpec as P


H = 8
KVH = 2
HD = 128
WINDOW = 128
CONV = 3
HALO = 16


SWAP = [(0, 1), (1, 0)]


def send(cells, axis, pairs):
    return lax.ppermute(cells, axis, pairs)


def xor_pairs(count, mask):
    return [(i, i ^ mask) for i in range(count)]


def attend(queries, keys, values, sink):
    tokens = queries.shape[0]
    heads_here = sink.shape[0]
    levels = lax.axis_size("sp")
    group = H // KVH
    scale = HD ** (-0.5)
    kv_head = (lax.axis_index("tp") * heads_here) // group
    own_keys = lax.dynamic_slice_in_dim(keys, kv_head * HD, HD, 1)
    own_values = lax.dynamic_slice_in_dim(values, kv_head * HD, HD, 1)
    both = jnp.stack([own_keys, own_values])
    up = [(i, i + 1) for i in range(levels - 1)]
    down = [(i + 1, i) for i in range(levels - 1)]
    before = send(both[:, tokens - WINDOW :], "sp", up)
    after = send(both[:, :WINDOW], "sp", down)
    extended = jnp.concatenate([before, both, after], axis=1)
    span = tokens + 2 * WINDOW
    q_heads = queries.reshape(tokens, heads_here, HD)
    scores = (
        jnp.einsum("qhd,kd->hqk", q_heads, extended[0], preferred_element_type=jnp.float32) * scale
    )
    offset = lax.axis_index("sp") * tokens
    q_pos = offset + jnp.arange(tokens, dtype=jnp.int32)[:, None]
    k_pos = offset - WINDOW + jnp.arange(span, dtype=jnp.int32)[None, :]
    valid = (jnp.abs(q_pos - k_pos) <= WINDOW) & (k_pos >= 0) & (k_pos < tokens * levels)
    scores = jnp.where(valid[None], scores, jnp.float32(-1e30))
    sink_col = sink[:, None]
    top = jnp.maximum(jnp.max(scores, axis=-1), sink_col)
    expo = jnp.exp(scores - top[..., None])
    total = jnp.sum(expo, axis=-1) + jnp.exp(sink_col - top)
    weights = (expo / total[..., None]).astype(jnp.bfloat16)
    mixed = jnp.einsum("hqk,kd->qhd", weights, extended[1], preferred_element_type=jnp.float32)
    return mixed.astype(jnp.bfloat16).reshape(tokens, heads_here * HD)


def gather_tp(block):
    count = lax.axis_size("tp")
    slots = {0: block}
    mask = count // 2
    while mask:
        for j in sorted(slots):
            slots[j ^ mask] = send(slots[j], "tp", xor_pairs(count, mask))
        mask //= 2
    return slots


def side_by_side(slots):
    count, tp = lax.axis_size("tp"), lax.axis_index("tp")
    rows, cols = slots[0].shape
    full = jnp.zeros((rows, count * cols), slots[0].dtype)
    for j, block in slots.items():
        full = lax.dynamic_update_slice(full, block, (0, (tp ^ j) * cols))
    return full


def normalize(queries, keys, values, sink, resid, out_proj, norm_gain):
    _, width = resid.shape
    count, tp = lax.axis_size("tp"), lax.axis_index("tp")
    cols = width // count
    mixed = attend(queries, keys, values, sink)
    all_heads = side_by_side(gather_tp(mixed))
    resid_own = lax.dynamic_slice_in_dim(resid, tp * cols, cols, 1)
    gain_own = lax.dynamic_slice_in_dim(norm_gain, tp * cols, cols, 0)
    summed = resid_own.astype(jnp.float32) + jnp.dot(
        all_heads, out_proj, preferred_element_type=jnp.float32
    )
    sums = jnp.stack([jnp.sum(summed, axis=-1), jnp.sum(summed * summed, axis=-1)])
    totals = sums
    for j in range(1, count):
        totals = totals + send(sums, "tp", xor_pairs(count, j))
    mean = (totals[0] / width)[:, None]
    msq = (totals[1] / width)[:, None]
    return ((summed - mean) * lax.rsqrt(msq - mean * mean + 1e-05) * gain_own).astype(
        jnp.bfloat16
    )


def shards(
    queries, keys, values, sink, resid, out_proj, norm_gain, w_gate, w_up, conv_w, conv_b, w_down
):
    fits = lax.axis_size("sp") == lax.axis_size("tp") == 4 and lax.axis_size("grp") == 2
    run = layer_of_four if fits else layer
    return run(
        queries, keys, values, sink, resid, out_proj, norm_gain,
        w_gate, w_up, conv_w, conv_b, w_down,
    )


def spread(full, piece_of, put):
    levels, level, part = lax.axis_size("sp"), lax.axis_index("sp"), lax.axis_index("grp")
    side = level // (levels // 2)
    for share in range(2):
        full = put(full, piece_of(side, share), level, share)
    for mask in range(1, levels):
        cells = piece_of((level ^ mask) // (levels // 2), part)
        got = send(cells, "sp", xor_pairs(levels, mask))
        other = send(got, "grp", SWAP)
        full = put(full, got, level ^ mask, part)
        full = put(full, other, level ^ mask, 1 - part)
    return full


def layer(
    queries, keys, values, sink, resid, out_proj, norm_gain, w_gate, w_up, conv_w, conv_b, w_down
):
    tokens = queries.shape[0]
    width = resid.shape[1]
    levels = lax.axis_size("sp")
    count = lax.axis_size("tp")
    level = lax.axis_index("sp")
    tp = lax.axis_index("tp")
    side = level // (levels // 2)
    cols = width // count
    rows_lv = width // levels
    half = w_gate.shape[1] // 2
    quarter = half // 2

    def gu_piece(of_side, share):
        rows = rows_lv // 2
        return jnp.concatenate(
            [
                lax.dynamic_slice(w, (share * rows, of_side * half), (rows, half))
                for w in (w_gate, w_up)
            ],
            axis=1,
        )

    def put_gu(full, piece, origin, share):
        return lax.dynamic_update_slice(full, piece[None, None], (origin, share, 0, 0))

    def d_piece(of_side, share):
        return lax.dynamic_slice(w_down, (of_side * half + share * quarter, 0), (quarter, rows_lv))

    per = levels // count

    def put_d(full, piece, origin, share):
        slot = (origin // per) ^ tp
        place = (slot >> 1) + (slot & 1) * (count // 2)
        return lax.dynamic_update_slice(
            full, piece[None, None], (place, share, 0, (origin % per) * rows_lv)
        )

    gu_full = jnp.zeros((levels, 2, rows_lv // 2, 2 * half), w_gate.dtype)
    gu_full = spread(gu_full, gu_piece, put_gu)
    gu_full = gu_full.reshape(width, 2 * half)
    d_full = jnp.zeros((count, 2, quarter, cols), w_down.dtype)
    d_full = spread(d_full, d_piece, put_d)
    d_full = d_full.reshape(count, half, cols)

    normed = normalize(queries, keys, values, sink, resid, out_proj, norm_gain)

    mate = levels // 2
    up = [(i, i + 1) for i in range(levels - 1)]
    down = [(i + 1, i) for i in range(levels - 1)]
    tail, head = normed[tokens - HALO :], normed[:HALO]
    other = send(normed, "sp", xor_pairs(levels, mate))
    own_before = send(tail, "sp", up)
    own_after = send(head, "sp", down)
    other_before = send(tail, "sp", [(a, b ^ mate) for a, b in up])
    other_after = send(head, "sp", [(a, b ^ mate) for a, b in down])
    pack = jnp.concatenate([other_before, other, other_after, own_before, own_after])
    normed_own = side_by_side(gather_tp(normed))
    normed_pack = side_by_side(gather_tp(pack))

    taps = lax.dynamic_slice_in_dim(conv_w, side * half, half, 1)
    bias = lax.dynamic_slice_in_dim(conv_b, side * half, half, 0)
    own_gu = jnp.dot(normed_own, gu_full, preferred_element_type=jnp.float32).astype(jnp.bfloat16)
    pack_gu = jnp.dot(normed_pack, gu_full, preferred_element_type=jnp.float32).astype(
        jnp.bfloat16
    )
    around = tokens + 2 * HALO

    def activate(gate, up_part):
        first = HALO - CONV // 2
        conv = bias
        for tap in range(CONV):
            conv = conv + gate[first + tap : first + tap + tokens].astype(jnp.float32) * taps[tap]
        return (jax.nn.silu(conv) * up_part.astype(jnp.float32)).astype(jnp.bfloat16)

    own_gate = jnp.concatenate(
        [pack_gu[around : around + HALO, :half], own_gu[:, :half], pack_gu[around + HALO :, :half]]
    )
    act_own = activate(own_gate, own_gu[:, half:])
    act_other = activate(pack_gu[:around, :half], pack_gu[HALO : HALO + tokens, half:])

    def partial(act, place):
        return jnp.dot(act, d_full[place], preferred_element_type=jnp.float32)

    def over_tp(act):
        pairs_here = count // 2
        away = [partial(act, pairs_here + i).astype(jnp.bfloat16) for i in range(pairs_here)]
        came = send(jnp.stack(away), "tp", xor_pairs(count, 1))
        here = [partial(act, i) + came[i].astype(jnp.float32) for i in range(pairs_here)]
        total = here[0]
        for i in range(1, pairs_here):
            block = send(here[i].astype(jnp.bfloat16), "tp", xor_pairs(count, 2 * i))
            total = total + block.astype(jnp.float32)
        return total

    sum_other = over_tp(act_other).astype(jnp.bfloat16)
    back = send(sum_other, "sp", xor_pairs(levels, mate))
    sum_own = over_tp(act_own)
    return (normed.astype(jnp.float32) + sum_own + back.astype(jnp.float32)).astype(jnp.bfloat16)


def gate_up_kernel(
    x0, x1, x2, x3, o0, o1, o2, o3, e0, e1, e2, e3, w_gate, w_up, z1, y1, z2, y2,
    acc, around, last, xs, es, ws, sems,
):
    tokens, cols = x0.shape
    half = acc.shape[1] // 2
    rows = z1.shape[0]
    level, tp, part = lax.axis_index("sp"), lax.axis_index("tp"), lax.axis_index("grp")
    odd = level & 1
    copies = []

    def copy(source, target):
        item = pltpu.make_async_copy(source, target, sems.at[len(copies)])
        item.start()
        copies.append(item)

    own_rows = pl.ds(pl.multiple_of(odd * tokens, tokens), tokens)
    other_rows = pl.ds(pl.multiple_of((1 - odd) * tokens, tokens), tokens)
    columns = ((x0, o0, e0), (x1, o1, e1), (x2, o2, e2), (x3, o3, e3))
    for j, (mine, other, edge) in enumerate(columns):
        lanes = pl.ds(pl.multiple_of((tp ^ j ^ level) * cols, cols), cols)
        copy(mine, xs.at[own_rows, lanes])
        copy(other, xs.at[other_rows, lanes])
        copy(edge, es.at[:, lanes])
    for i, w in enumerate((w_gate, w_up)):
        copy(
            w.at[:, pl.ds(pl.multiple_of(odd * half, half), half)],
            ws.at[0:cols, i * half : (i + 1) * half],
        )
    for mask, (z, y) in enumerate(((z1, y1), (z2, y2)), 1):
        base = mask * cols
        copy(z, ws.at[pl.ds(pl.multiple_of(base + part * rows, rows), rows), :])
        copy(y, ws.at[pl.ds(pl.multiple_of(base + (1 - part) * rows, rows), rows), :])
    for item in copies:
        item.wait()
    known = 3 * cols
    around[...] = jnp.dot(es[:, :known], ws[:, :half], preferred_element_type=jnp.float32)
    last[0 : 2 * tokens, :] = xs[:, known:]
    last[2 * tokens : 2 * tokens + 2 * HALO, :] = es[:, known:]
    step = 256

    def some_rows(i, carry):
        here = pl.ds(pl.multiple_of(i * step, step), step)
        acc[here, :] = jnp.dot(xs[here, :known], ws[...], preferred_element_type=jnp.float32)
        return carry

    lax.fori_loop(0, 2 * tokens // step, some_rows, 0)


def gate_up(own, other, edges, w_gate, w_up, pieces):
    tokens, cols = own[0].shape
    both = w_gate.shape[1]
    near, far = pl.BlockSpec(memory_space=pl.ANY), pl.BlockSpec(memory_space=pltpu.VMEM)
    return pl.pallas_call(
        gate_up_kernel,
        out_shape=(
            jax.ShapeDtypeStruct((2 * tokens, both), jnp.float32),
            jax.ShapeDtypeStruct((2 * HALO, both // 2), jnp.float32),
            jax.ShapeDtypeStruct((2 * tokens + 2 * HALO, cols), jnp.bfloat16),
        ),
        in_specs=[near] * 18,
        out_specs=(far, far, far),
        scratch_shapes=[
            pltpu.VMEM((2 * tokens, 4 * cols), jnp.bfloat16),
            pltpu.VMEM((2 * HALO, 4 * cols), jnp.bfloat16),
            pltpu.VMEM((3 * cols, both), jnp.bfloat16),
            pltpu.SemaphoreType.DMA((18,)),
        ],
        compiler_params=pltpu.CompilerParams(vmem_limit_bytes=32 * 2**20),
        name="gate_up",
    )(*own, *other, *edges, w_gate, w_up, *pieces)


def activate_kernel(acc, around, last, z3, y3, taps, bias, out, ws, gate, sems):
    tokens2, both = acc.shape
    half = both // 2
    rows = z3.shape[0]
    level, part = lax.axis_index("sp"), lax.axis_index("grp")
    copies = [
        pltpu.make_async_copy(
            source, ws.at[pl.ds(pl.multiple_of(share * rows, rows), rows), :], sems.at[i]
        )
        for i, (source, share) in enumerate(((z3, part), (y3, 1 - part)))
    ]
    for item in copies:
        item.start()
    for item in copies:
        item.wait()
    step = 256
    ends = around[...] + jnp.dot(
        last[tokens2:, :], ws[:, :half], preferred_element_type=jnp.float32
    )
    ends = ends.astype(jnp.bfloat16).astype(jnp.float32)
    even = (level & 1) == 0
    gate[7:8, :] = jnp.where(even, ends[HALO - 1 : HALO], ends[2 * HALO - 1 : 2 * HALO])
    gate[8 + tokens2 : 9 + tokens2, :] = jnp.where(even, ends[HALO : HALO + 1], ends[0:1])

    def gates(i, carry):
        here = pl.ds(pl.multiple_of(i * step, step), step)
        total = acc[here, :half] + jnp.dot(
            last[here, :], ws[:, :half], preferred_element_type=jnp.float32
        )
        gate[pl.ds(pl.multiple_of(8 + i * step, 8), step), :] = total.astype(jnp.bfloat16).astype(
            jnp.float32
        )
        return carry

    lax.fori_loop(0, tokens2 // step, gates, 0)
    for start in range(0, tokens2, step):
        here = slice(start, start + step)
        total = acc[here, half:] + jnp.dot(
            last[here, :], ws[:, half:], preferred_element_type=jnp.float32
        )
        up_part = total.astype(jnp.bfloat16).astype(jnp.float32)
        conv = bias[...]
        for tap in range(CONV):
            conv = conv + gate[7 + tap + start : 7 + tap + start + step, :] * taps[tap : tap + 1, :]
        silu = conv / (1.0 + jnp.exp(-conv))
        out[here, :] = (silu * up_part).astype(jnp.bfloat16)


def activate_last(sums, pieces, taps, bias):
    acc, around, last = sums
    near, far = pl.BlockSpec(memory_space=pl.ANY), pl.BlockSpec(memory_space=pltpu.VMEM)
    half = taps.shape[1]
    return pl.pallas_call(
        activate_kernel,
        out_shape=jax.ShapeDtypeStruct((acc.shape[0], half), jnp.bfloat16),
        in_specs=[far] * 3 + [near] * 2 + [far] * 2,
        out_specs=far,
        scratch_shapes=[
            pltpu.VMEM((last.shape[1], 2 * half), jnp.bfloat16),
            pltpu.VMEM((acc.shape[0] + HALO, half), jnp.float32),
            pltpu.SemaphoreType.DMA((2,)),
        ],
        compiler_params=pltpu.CompilerParams(vmem_limit_bytes=32 * 2**20),
        name="activate",
    )(acc, around, last, *pieces, taps, bias)


def place_of(slot):
    return (slot >> 1) + 2 * (slot & 1)


def down_kernel(act, w_down, z1, y1, z2, y2, away_other, away_own, here, ds, sems):
    tokens, _ = here.shape[2:]
    half = act.shape[1]
    quarter = half // 2
    level, tp, part = lax.axis_index("sp"), lax.axis_index("tp"), lax.axis_index("grp")
    odd = level & 1
    lower = pl.ds(pl.multiple_of(part * quarter, quarter), quarter)
    upper = pl.ds(pl.multiple_of((1 - part) * quarter, quarter), quarter)
    copies = []

    def copy(source, target):
        item = pltpu.make_async_copy(source, target, sems.at[len(copies)])
        item.start()
        copies.append(item)

    copy(
        w_down.at[pl.ds(pl.multiple_of(odd * half, half), half), :],
        ds.at[place_of(level ^ tp)],
    )
    for mask, (z, y) in enumerate(((z1, y1), (z2, y2)), 1):
        place = place_of(level ^ mask ^ tp)
        copy(z, ds.at[place, lower, :])
        copy(y, ds.at[place, upper, :])
    for item in copies:
        item.wait()
    for which, away in ((0, away_other), (1, away_own)):
        block = odd if which else 1 - odd
        cells = act[pl.ds(pl.multiple_of(block * tokens, tokens), tokens), :]
        for i in range(2):
            away[i] = jnp.dot(cells, ds[2 + i], preferred_element_type=jnp.float32).astype(
                away.dtype
            )
            here[which, i] = jnp.dot(cells, ds[i], preferred_element_type=jnp.float32).astype(
                here.dtype
            )


def down_last_kernel(
    act, z3, y3, away_other_in, away_own_in, here_in, away_other, away_own, here, ds, sums, sems
):
    del away_other_in, away_own_in, here_in
    tokens = sums.shape[1]
    half = act.shape[1]
    quarter = half // 2
    level, tp, part = lax.axis_index("sp"), lax.axis_index("tp"), lax.axis_index("grp")
    odd = level & 1
    slot = level ^ 3 ^ tp
    loads = [
        pltpu.make_async_copy(
            source, ds.at[pl.ds(pl.multiple_of(share * quarter, quarter), quarter), :], sems.at[i]
        )
        for i, (source, share) in enumerate(((z3, part), (y3, 1 - part)))
    ]
    for item in loads:
        item.start()
    for item in loads:
        item.wait()
    for which in range(2):
        block = odd if which else 1 - odd
        cells = act[pl.ds(pl.multiple_of(block * tokens, tokens), tokens), :]
        sums[which] = jnp.dot(cells, ds[...], preferred_element_type=jnp.float32).astype(sums.dtype)

    def store(targets):
        stores = [
            pltpu.make_async_copy(sums.at[which], target, sems.at[2 + which])
            for which, target in enumerate(targets)
        ]
        for item in stores:
            item.start()
        for item in stores:
            item.wait()

    @pl.when((slot & 1) == 1)
    def _():
        store((away_other.at[slot >> 1], away_own.at[slot >> 1]))

    @pl.when((slot & 1) == 0)
    def _():
        store((here.at[0, slot >> 1], here.at[1, slot >> 1]))


def down(act, w_down, pieces):
    tokens, half = act.shape[0] // 2, act.shape[1]
    cols = w_down.shape[1]
    near, far = pl.BlockSpec(memory_space=pl.ANY), pl.BlockSpec(memory_space=pltpu.VMEM)
    shapes = (
        jax.ShapeDtypeStruct((2, tokens, cols), jnp.bfloat16),
        jax.ShapeDtypeStruct((2, tokens, cols), jnp.bfloat16),
        jax.ShapeDtypeStruct((2, 2, tokens, cols), jnp.bfloat16),
    )
    known = pl.pallas_call(
        down_kernel,
        out_shape=shapes,
        in_specs=[far] + [near] * 5,
        out_specs=(far, far, far),
        scratch_shapes=[pltpu.VMEM((4, half, cols), jnp.bfloat16), pltpu.SemaphoreType.DMA((5,))],
        compiler_params=pltpu.CompilerParams(vmem_limit_bytes=24 * 2**20),
        name="down",
    )(act, w_down, *pieces[:4])
    return pl.pallas_call(
        down_last_kernel,
        out_shape=shapes,
        in_specs=[far] + [near] * 5,
        out_specs=(near, near, near),
        input_output_aliases={3: 0, 4: 1, 5: 2},
        scratch_shapes=[
            pltpu.VMEM((half, cols), jnp.bfloat16),
            pltpu.VMEM((2, tokens, cols), jnp.bfloat16),
            pltpu.SemaphoreType.DMA((4,)),
        ],
        compiler_params=pltpu.CompilerParams(vmem_limit_bytes=16 * 2**20),
        name="down_last",
    )(act, *pieces[4:], *known)


def travel(piece_of):
    odd, part = lax.axis_index("sp") & 1, lax.axis_index("grp")
    pieces = []
    for mask in range(1, 4):
        z = send(piece_of(odd ^ (mask & 1), part), "sp", xor_pairs(4, mask))
        pieces += [z, send(z, "grp", SWAP)]
    return pieces


def layer_of_four(
    queries, keys, values, sink, resid, out_proj, norm_gain, w_gate, w_up, conv_w, conv_b, w_down
):
    tokens = queries.shape[0]
    odd = lax.axis_index("sp") & 1
    half = w_gate.shape[1] // 2
    quarter = half // 2

    def gu_piece(of_side, share):
        rows = w_gate.shape[0] // 2
        return jnp.concatenate(
            [
                lax.dynamic_slice(w, (share * rows, of_side * half), (rows, half))
                for w in (w_gate, w_up)
            ],
            axis=1,
        )

    def d_piece(of_side, share):
        return lax.dynamic_slice(
            w_down, (of_side * half + share * quarter, 0), (quarter, w_down.shape[1])
        )

    gu = travel(gu_piece)
    dn = travel(d_piece)
    normed = normalize(queries, keys, values, sink, resid, out_proj, norm_gain)
    mate = send(normed, "sp", xor_pairs(4, 1))
    outer = jnp.where(odd == 1, normed[tokens - HALO :], normed[:HALO])
    near = send(outer, "sp", [(1, 2), (2, 1)])
    far = send(outer, "sp", [(1, 3), (2, 0)])
    own = gather_tp(normed)
    other = gather_tp(mate)
    edges = gather_tp(jnp.concatenate([near, far]))

    taps = lax.dynamic_slice_in_dim(conv_w, odd * half, half, 1)
    bias = lax.dynamic_slice_in_dim(conv_b, odd * half, half, 0)
    sums = gate_up(
        *([slots[j] for j in range(4)] for slots in (own, other, edges)), w_gate, w_up, gu[:4]
    )
    act = activate_last(sums, gu[4:], taps, bias[None])

    away_other, away_own, here = down(act, w_down, dn)
    came = [send(away_other, "tp", xor_pairs(4, 1)), send(away_own, "tp", xor_pairs(4, 1))]

    middle = tokens // 2

    def partial(which, slot, rows):
        return here[which, slot, rows].astype(jnp.float32) + came[which][slot, rows].astype(jnp.float32)

    def cross(cells, axis, mask):
        return send(cells.astype(jnp.bfloat16), axis, xor_pairs(4, mask)).astype(jnp.float32)

    top, low = slice(0, middle), slice(middle, tokens)
    x_other = cross(partial(0, 1, top), "tp", 2)
    z_low = cross(jnp.stack([partial(0, 0, low), partial(0, 1, low)]), "sp", 1)
    x_top = cross(partial(1, 1, top), "tp", 2)
    back = cross(partial(0, 0, top) + x_other, "sp", 1)
    low_sum = (partial(1, 1, low) + z_low[1]).astype(jnp.bfloat16)
    x_low = cross(low_sum, "tp", 2)
    ffn = jnp.concatenate([partial(1, 0, top) + x_top + back, partial(1, 0, low) + z_low[0] + x_low])
    return (normed.astype(jnp.float32) + ffn).astype(jnp.bfloat16)


def solution(mesh):
    step = jax.shard_map(
        shards,
        mesh=mesh,
        in_specs=(
            P(("grp", "sp"), "tp"),
            P(("grp", "sp"), None),
            P(("grp", "sp"), None),
            P("tp"),
            P(("grp", "sp"), None),
            P(None, "tp"),
            P(),
            P("sp", "tp"),
            P("sp", "tp"),
            P(None, "tp"),
            P("tp"),
            P("tp", "sp"),
        ),
        out_specs=P(("grp", "sp"), "tp"),
        check_vma=False,
    )
    if not (mesh.shape["sp"] == mesh.shape["tp"] == 4 and mesh.shape["grp"] == 2):
        return step
    return step
```

```python
import jax
import jax.numpy as jnp
from jax import lax
from jax.experimental import pallas as pl
from jax.experimental.pallas import tpu as pltpu
from jax.sharding import PartitionSpec as P


H = 8
KVH = 2
HD = 128
WINDOW = 128
CONV = 3
HALO = 16
MIDDLE = 9


SWAP = [(0, 1), (1, 0)]


def send(cells, axis, pairs):
    return lax.ppermute(cells, axis, pairs)


def xor_pairs(count, mask):
    return [(i, i ^ mask) for i in range(count)]


def attend(queries, keys, values, sink):
    tokens = queries.shape[0]
    heads_here = sink.shape[0]
    levels = lax.axis_size("sp")
    group = H // KVH
    scale = HD ** (-0.5)
    kv_head = (lax.axis_index("tp") * heads_here) // group
    own_keys = lax.dynamic_slice_in_dim(keys, kv_head * HD, HD, 1)
    own_values = lax.dynamic_slice_in_dim(values, kv_head * HD, HD, 1)
    both = jnp.stack([own_keys, own_values])
    up = [(i, i + 1) for i in range(levels - 1)]
    down = [(i + 1, i) for i in range(levels - 1)]

    def rows_of(start):
        return jnp.stack(
            [lax.dynamic_slice(cells, (start, kv_head * HD), (WINDOW, HD)) for cells in (keys, values)]
        )

    before = send(rows_of(tokens - WINDOW), "sp", up)
    after = send(rows_of(0), "sp", down)
    extended = jnp.concatenate([before, both, after], axis=1)
    span = tokens + 2 * WINDOW
    q_heads = queries.reshape(tokens, heads_here, HD)
    scores = (
        jnp.einsum("qhd,kd->hqk", q_heads, extended[0], preferred_element_type=jnp.float32) * scale
    )
    offset = lax.axis_index("sp") * tokens
    q_pos = offset + jnp.arange(tokens, dtype=jnp.int32)[:, None]
    k_pos = offset - WINDOW + jnp.arange(span, dtype=jnp.int32)[None, :]
    valid = (jnp.abs(q_pos - k_pos) <= WINDOW) & (k_pos >= 0) & (k_pos < tokens * levels)
    scores = jnp.where(valid[None], scores, jnp.float32(-1e30))
    sink_col = sink[:, None]
    top = jnp.maximum(jnp.max(scores, axis=-1), sink_col)
    expo = jnp.exp(scores - top[..., None])
    total = jnp.sum(expo, axis=-1) + jnp.exp(sink_col - top)
    weights = (expo / total[..., None]).astype(jnp.bfloat16)
    mixed = jnp.einsum("hqk,kd->qhd", weights, extended[1], preferred_element_type=jnp.float32)
    return mixed.astype(jnp.bfloat16).reshape(tokens, heads_here * HD)


def gather_tp(block):
    count = lax.axis_size("tp")
    slots = {0: block}
    mask = count // 2
    while mask:
        for j in sorted(slots):
            slots[j ^ mask] = send(slots[j], "tp", xor_pairs(count, mask))
        mask //= 2
    return slots


def side_by_side(slots):
    count, tp = lax.axis_size("tp"), lax.axis_index("tp")
    rows, cols = slots[0].shape
    full = jnp.zeros((rows, count * cols), slots[0].dtype)
    for j, block in slots.items():
        full = lax.dynamic_update_slice(full, block, (0, (tp ^ j) * cols))
    return full


def normalize(queries, keys, values, sink, resid, out_proj, norm_gain):
    _, width = resid.shape
    count, tp = lax.axis_size("tp"), lax.axis_index("tp")
    cols = width // count
    mixed = attend(queries, keys, values, sink)
    all_heads = side_by_side(gather_tp(mixed))
    resid_own = lax.dynamic_slice_in_dim(resid, tp * cols, cols, 1)
    gain_own = lax.dynamic_slice_in_dim(norm_gain, tp * cols, cols, 0)
    summed = resid_own.astype(jnp.float32) + jnp.dot(
        all_heads, out_proj, preferred_element_type=jnp.float32
    )
    sums = jnp.stack([jnp.sum(summed, axis=-1), jnp.sum(summed * summed, axis=-1)])
    totals = sums
    for j in range(1, count):
        totals = totals + send(sums, "tp", xor_pairs(count, j))
    mean = (totals[0] / width)[:, None]
    msq = (totals[1] / width)[:, None]
    return ((summed - mean) * lax.rsqrt(msq - mean * mean + 1e-05) * gain_own).astype(
        jnp.bfloat16
    )


def shards(
    queries, keys, values, sink, resid, out_proj, norm_gain, w_gate, w_up, conv_w, conv_b, w_down
):
    fits = lax.axis_size("sp") == lax.axis_size("tp") == 4 and lax.axis_size("grp") == 2
    run = layer_of_four if fits else layer
    return run(
        queries, keys, values, sink, resid, out_proj, norm_gain,
        w_gate, w_up, conv_w, conv_b, w_down,
    )


def spread(full, piece_of, put):
    levels, level, part = lax.axis_size("sp"), lax.axis_index("sp"), lax.axis_index("grp")
    side = level // (levels // 2)
    for share in range(2):
        full = put(full, piece_of(side, share), level, share)
    for mask in range(1, levels):
        cells = piece_of((level ^ mask) // (levels // 2), part)
        got = send(cells, "sp", xor_pairs(levels, mask))
        other = send(got, "grp", SWAP)
        full = put(full, got, level ^ mask, part)
        full = put(full, other, level ^ mask, 1 - part)
    return full


def layer(
    queries, keys, values, sink, resid, out_proj, norm_gain, w_gate, w_up, conv_w, conv_b, w_down
):
    tokens = queries.shape[0]
    width = resid.shape[1]
    levels = lax.axis_size("sp")
    count = lax.axis_size("tp")
    level = lax.axis_index("sp")
    tp = lax.axis_index("tp")
    side = level // (levels // 2)
    cols = width // count
    rows_lv = width // levels
    half = w_gate.shape[1] // 2
    quarter = half // 2

    def gu_piece(of_side, share):
        rows = rows_lv // 2
        return jnp.concatenate(
            [
                lax.dynamic_slice(w, (share * rows, of_side * half), (rows, half))
                for w in (w_gate, w_up)
            ],
            axis=1,
        )

    def put_gu(full, piece, origin, share):
        return lax.dynamic_update_slice(full, piece[None, None], (origin, share, 0, 0))

    def d_piece(of_side, share):
        return lax.dynamic_slice(w_down, (of_side * half + share * quarter, 0), (quarter, rows_lv))

    per = levels // count

    def put_d(full, piece, origin, share):
        slot = (origin // per) ^ tp
        place = (slot >> 1) + (slot & 1) * (count // 2)
        return lax.dynamic_update_slice(
            full, piece[None, None], (place, share, 0, (origin % per) * rows_lv)
        )

    gu_full = jnp.zeros((levels, 2, rows_lv // 2, 2 * half), w_gate.dtype)
    gu_full = spread(gu_full, gu_piece, put_gu)
    gu_full = gu_full.reshape(width, 2 * half)
    d_full = jnp.zeros((count, 2, quarter, cols), w_down.dtype)
    d_full = spread(d_full, d_piece, put_d)
    d_full = d_full.reshape(count, half, cols)

    normed = normalize(queries, keys, values, sink, resid, out_proj, norm_gain)

    mate = levels // 2
    up = [(i, i + 1) for i in range(levels - 1)]
    down = [(i + 1, i) for i in range(levels - 1)]
    tail, head = normed[tokens - HALO :], normed[:HALO]
    other = send(normed, "sp", xor_pairs(levels, mate))
    own_before = send(tail, "sp", up)
    own_after = send(head, "sp", down)
    other_before = send(tail, "sp", [(a, b ^ mate) for a, b in up])
    other_after = send(head, "sp", [(a, b ^ mate) for a, b in down])
    pack = jnp.concatenate([other_before, other, other_after, own_before, own_after])
    normed_own = side_by_side(gather_tp(normed))
    normed_pack = side_by_side(gather_tp(pack))

    taps = lax.dynamic_slice_in_dim(conv_w, side * half, half, 1)
    bias = lax.dynamic_slice_in_dim(conv_b, side * half, half, 0)
    own_gu = jnp.dot(normed_own, gu_full, preferred_element_type=jnp.float32).astype(jnp.bfloat16)
    pack_gu = jnp.dot(normed_pack, gu_full, preferred_element_type=jnp.float32).astype(
        jnp.bfloat16
    )
    around = tokens + 2 * HALO

    def activate(gate, up_part):
        first = HALO - CONV // 2
        conv = bias
        for tap in range(CONV):
            conv = conv + gate[first + tap : first + tap + tokens].astype(jnp.float32) * taps[tap]
        return (jax.nn.silu(conv) * up_part.astype(jnp.float32)).astype(jnp.bfloat16)

    own_gate = jnp.concatenate(
        [pack_gu[around : around + HALO, :half], own_gu[:, :half], pack_gu[around + HALO :, :half]]
    )
    act_own = activate(own_gate, own_gu[:, half:])
    act_other = activate(pack_gu[:around, :half], pack_gu[HALO : HALO + tokens, half:])

    def partial(act, place):
        return jnp.dot(act, d_full[place], preferred_element_type=jnp.float32)

    def over_tp(act):
        pairs_here = count // 2
        away = [partial(act, pairs_here + i).astype(jnp.bfloat16) for i in range(pairs_here)]
        came = send(jnp.stack(away), "tp", xor_pairs(count, 1))
        here = [partial(act, i) + came[i].astype(jnp.float32) for i in range(pairs_here)]
        total = here[0]
        for i in range(1, pairs_here):
            block = send(here[i].astype(jnp.bfloat16), "tp", xor_pairs(count, 2 * i))
            total = total + block.astype(jnp.float32)
        return total

    sum_other = over_tp(act_other).astype(jnp.bfloat16)
    back = send(sum_other, "sp", xor_pairs(levels, mate))
    sum_own = over_tp(act_own)
    return (normed.astype(jnp.float32) + sum_own + back.astype(jnp.float32)).astype(jnp.bfloat16)


def gate_up_kernel(
    x0, x1, x2, x3, o0, o1, o2, o3, e0, e1, e2, e3, w_gate, w_up, z1, y1, z2, y2,
    acc, around, last, xs, es, ws, sems,
):
    tokens, cols = x0.shape
    half = acc.shape[1] // 2
    rows = z1.shape[0]
    level, tp, part = lax.axis_index("sp"), lax.axis_index("tp"), lax.axis_index("grp")
    odd = level & 1
    copies = []

    def copy(source, target):
        item = pltpu.make_async_copy(source, target, sems.at[len(copies)])
        item.start()
        copies.append(item)

    own_rows = pl.ds(pl.multiple_of(odd * tokens, tokens), tokens)
    other_rows = pl.ds(pl.multiple_of((1 - odd) * tokens, tokens), tokens)
    columns = ((x0, o0, e0), (x1, o1, e1), (x2, o2, e2), (x3, o3, e3))
    for j, (mine, other, edge) in enumerate(columns):
        lanes = pl.ds(pl.multiple_of((tp ^ j ^ level) * cols, cols), cols)
        copy(mine, xs.at[own_rows, lanes])
        copy(other, xs.at[other_rows, lanes])
        copy(edge, es.at[:, lanes])
    for i, w in enumerate((w_gate, w_up)):
        copy(
            w.at[:, pl.ds(pl.multiple_of(odd * half, half), half)],
            ws.at[0:cols, i * half : (i + 1) * half],
        )
    for mask, (z, y) in enumerate(((z1, y1), (z2, y2)), 1):
        base = mask * cols
        copy(z, ws.at[pl.ds(pl.multiple_of(base + part * rows, rows), rows), :])
        copy(y, ws.at[pl.ds(pl.multiple_of(base + (1 - part) * rows, rows), rows), :])
    for item in copies:
        item.wait()
    known = 3 * cols
    around[...] = jnp.dot(es[:, :known], ws[:, :half], preferred_element_type=jnp.float32)
    last[0 : 2 * tokens, :] = xs[:, known:]
    last[2 * tokens : 2 * tokens + 2 * HALO, :] = es[:, known:]
    step = 256

    def some_rows(i, carry):
        here = pl.ds(pl.multiple_of(i * step, step), step)
        acc[here, :] = jnp.dot(xs[here, :known], ws[...], preferred_element_type=jnp.float32)
        return carry

    lax.fori_loop(0, 2 * tokens // step, some_rows, 0)


def gate_up(own, other, edges, w_gate, w_up, pieces):
    tokens, cols = own[0].shape
    both = w_gate.shape[1]
    near, far = pl.BlockSpec(memory_space=pl.ANY), pl.BlockSpec(memory_space=pltpu.VMEM)
    return pl.pallas_call(
        gate_up_kernel,
        out_shape=(
            jax.ShapeDtypeStruct((2 * tokens, both), jnp.float32),
            jax.ShapeDtypeStruct((2 * HALO, both // 2), jnp.float32),
            jax.ShapeDtypeStruct((2 * tokens + 2 * HALO, cols), jnp.bfloat16),
        ),
        in_specs=[near] * 18,
        out_specs=(far, far, far),
        scratch_shapes=[
            pltpu.VMEM((2 * tokens, 4 * cols), jnp.bfloat16),
            pltpu.VMEM((2 * HALO, 4 * cols), jnp.bfloat16),
            pltpu.VMEM((3 * cols, both), jnp.bfloat16),
            pltpu.SemaphoreType.DMA((18,)),
        ],
        compiler_params=pltpu.CompilerParams(vmem_limit_bytes=32 * 2**20),
        name="gate_up",
    )(*own, *other, *edges, w_gate, w_up, *pieces)


def activate_kernel(acc, around, last, z3, y3, taps, bias, out, ws, gate, sems):
    tokens2, both = acc.shape
    half = both // 2
    rows = z3.shape[0]
    level, part = lax.axis_index("sp"), lax.axis_index("grp")
    copies = [
        pltpu.make_async_copy(
            source, ws.at[pl.ds(pl.multiple_of(share * rows, rows), rows), :], sems.at[i]
        )
        for i, (source, share) in enumerate(((z3, part), (y3, 1 - part)))
    ]
    for item in copies:
        item.start()
    for item in copies:
        item.wait()
    step = 256
    ends = around[...] + jnp.dot(
        last[tokens2:, :], ws[:, :half], preferred_element_type=jnp.float32
    )
    ends = ends.astype(jnp.bfloat16).astype(jnp.float32)
    even = (level & 1) == 0
    gate[7:8, :] = jnp.where(even, ends[HALO - 1 : HALO], ends[2 * HALO - 1 : 2 * HALO])
    gate[8 + tokens2 : 9 + tokens2, :] = jnp.where(even, ends[HALO : HALO + 1], ends[0:1])

    def gates(i, carry):
        here = pl.ds(pl.multiple_of(i * step, step), step)
        total = acc[here, :half] + jnp.dot(
            last[here, :], ws[:, :half], preferred_element_type=jnp.float32
        )
        gate[pl.ds(pl.multiple_of(8 + i * step, 8), step), :] = total.astype(jnp.bfloat16).astype(
            jnp.float32
        )
        return carry

    lax.fori_loop(0, tokens2 // step, gates, 0)
    for start in range(0, tokens2, step):
        here = slice(start, start + step)
        total = acc[here, half:] + jnp.dot(
            last[here, :], ws[:, half:], preferred_element_type=jnp.float32
        )
        up_part = total.astype(jnp.bfloat16).astype(jnp.float32)
        conv = bias[...]
        for tap in range(CONV):
            conv = conv + gate[7 + tap + start : 7 + tap + start + step, :] * taps[tap : tap + 1, :]
        silu = conv / (1.0 + jnp.exp(-conv))
        out[here, :] = (silu * up_part).astype(jnp.bfloat16)


def activate_last(sums, pieces, taps, bias):
    acc, around, last = sums
    near, far = pl.BlockSpec(memory_space=pl.ANY), pl.BlockSpec(memory_space=pltpu.VMEM)
    half = taps.shape[1]
    return pl.pallas_call(
        activate_kernel,
        out_shape=jax.ShapeDtypeStruct((acc.shape[0], half), jnp.bfloat16),
        in_specs=[far] * 3 + [near] * 2 + [far] * 2,
        out_specs=far,
        scratch_shapes=[
            pltpu.VMEM((last.shape[1], 2 * half), jnp.bfloat16),
            pltpu.VMEM((acc.shape[0] + HALO, half), jnp.float32),
            pltpu.SemaphoreType.DMA((2,)),
        ],
        compiler_params=pltpu.CompilerParams(vmem_limit_bytes=32 * 2**20),
        name="activate",
    )(acc, around, last, *pieces, taps, bias)


def place_of(slot):
    return (slot >> 1) + 2 * (slot & 1)


def down_kernel(act, w_down, z1, y1, z2, y2, away_other, away_own, here, ds, sems):
    tokens, _ = here.shape[2:]
    half = act.shape[1]
    quarter = half // 2
    level, tp, part = lax.axis_index("sp"), lax.axis_index("tp"), lax.axis_index("grp")
    odd = level & 1
    lower = pl.ds(pl.multiple_of(part * quarter, quarter), quarter)
    upper = pl.ds(pl.multiple_of((1 - part) * quarter, quarter), quarter)
    copies = []

    def copy(source, target):
        item = pltpu.make_async_copy(source, target, sems.at[len(copies)])
        item.start()
        copies.append(item)

    copy(
        w_down.at[pl.ds(pl.multiple_of(odd * half, half), half), :],
        ds.at[place_of(level ^ tp)],
    )
    for mask, (z, y) in enumerate(((z1, y1), (z2, y2)), 1):
        place = place_of(level ^ mask ^ tp)
        copy(z, ds.at[place, lower, :])
        copy(y, ds.at[place, upper, :])
    for item in copies:
        item.wait()
    for which, away in ((0, away_other), (1, away_own)):
        block = odd if which else 1 - odd
        cells = act[pl.ds(pl.multiple_of(block * tokens, tokens), tokens), :]
        for i in range(2):
            away[i] = jnp.dot(cells, ds[2 + i], preferred_element_type=jnp.float32).astype(
                away.dtype
            )
            here[which, i] = jnp.dot(cells, ds[i], preferred_element_type=jnp.float32).astype(
                here.dtype
            )


def down_last_kernel(
    act, z3, y3, away_other_in, away_own_in, here_in, away_other, away_own, here, ds, sums, sems
):
    del away_other_in, away_own_in, here_in
    tokens = sums.shape[1]
    half = act.shape[1]
    quarter = half // 2
    level, tp, part = lax.axis_index("sp"), lax.axis_index("tp"), lax.axis_index("grp")
    odd = level & 1
    slot = level ^ 3 ^ tp
    loads = [
        pltpu.make_async_copy(
            source, ds.at[pl.ds(pl.multiple_of(share * quarter, quarter), quarter), :], sems.at[i]
        )
        for i, (source, share) in enumerate(((z3, part), (y3, 1 - part)))
    ]
    for item in loads:
        item.start()
    for item in loads:
        item.wait()
    for which in range(2):
        block = odd if which else 1 - odd
        cells = act[pl.ds(pl.multiple_of(block * tokens, tokens), tokens), :]
        sums[which] = jnp.dot(cells, ds[...], preferred_element_type=jnp.float32).astype(sums.dtype)

    def store(targets):
        stores = [
            pltpu.make_async_copy(sums.at[which], target, sems.at[2 + which])
            for which, target in enumerate(targets)
        ]
        for item in stores:
            item.start()
        for item in stores:
            item.wait()

    @pl.when((slot & 1) == 1)
    def _():
        store((away_other.at[slot >> 1], away_own.at[slot >> 1]))

    @pl.when((slot & 1) == 0)
    def _():
        store((here.at[0, slot >> 1], here.at[1, slot >> 1]))


def down(act, w_down, pieces):
    tokens, half = act.shape[0] // 2, act.shape[1]
    cols = w_down.shape[1]
    near, far = pl.BlockSpec(memory_space=pl.ANY), pl.BlockSpec(memory_space=pltpu.VMEM)
    shapes = (
        jax.ShapeDtypeStruct((2, tokens, cols), jnp.bfloat16),
        jax.ShapeDtypeStruct((2, tokens, cols), jnp.bfloat16),
        jax.ShapeDtypeStruct((2, 2, tokens, cols), jnp.bfloat16),
    )
    known = pl.pallas_call(
        down_kernel,
        out_shape=shapes,
        in_specs=[far] + [near] * 5,
        out_specs=(far, far, far),
        scratch_shapes=[pltpu.VMEM((4, half, cols), jnp.bfloat16), pltpu.SemaphoreType.DMA((5,))],
        compiler_params=pltpu.CompilerParams(vmem_limit_bytes=24 * 2**20),
        name="down",
    )(act, w_down, *pieces[:4])
    return pl.pallas_call(
        down_last_kernel,
        out_shape=shapes,
        in_specs=[far] + [near] * 5,
        out_specs=(near, near, near),
        input_output_aliases={3: 0, 4: 1, 5: 2},
        scratch_shapes=[
            pltpu.VMEM((half, cols), jnp.bfloat16),
            pltpu.VMEM((2, tokens, cols), jnp.bfloat16),
            pltpu.SemaphoreType.DMA((4,)),
        ],
        compiler_params=pltpu.CompilerParams(vmem_limit_bytes=16 * 2**20),
        name="down_last",
    )(act, *pieces[4:], *known)


def travel(piece_of):
    odd, part = lax.axis_index("sp") & 1, lax.axis_index("grp")
    pieces = []
    for mask in range(1, 4):
        z = send(piece_of(odd ^ (mask & 1), part), "sp", xor_pairs(4, mask))
        pieces += [z, send(z, "grp", SWAP)]
    return pieces


def layer_of_four(
    queries, keys, values, sink, resid, out_proj, norm_gain, w_gate, w_up, conv_w, conv_b, w_down
):
    tokens = queries.shape[0]
    odd = lax.axis_index("sp") & 1
    half = w_gate.shape[1] // 2
    quarter = half // 2

    def gu_piece(of_side, share):
        rows = w_gate.shape[0] // 2
        return jnp.concatenate(
            [
                lax.dynamic_slice(w, (share * rows, of_side * half), (rows, half))
                for w in (w_gate, w_up)
            ],
            axis=1,
        )

    def d_piece(of_side, share):
        return lax.dynamic_slice(
            w_down, (of_side * half + share * quarter, 0), (quarter, w_down.shape[1])
        )

    gu = travel(gu_piece)
    dn = travel(d_piece)
    normed = normalize(queries, keys, values, sink, resid, out_proj, norm_gain)
    mate = send(normed, "sp", xor_pairs(4, 1))
    outer = jnp.where(odd == 1, normed[tokens - HALO :], normed[:HALO])
    near = send(outer, "sp", [(1, 2), (2, 1)])
    far = send(outer, "sp", [(1, 3), (2, 0)])
    own = gather_tp(normed)
    other = gather_tp(mate)
    edges = gather_tp(jnp.concatenate([near, far]))

    taps = lax.dynamic_slice_in_dim(conv_w, odd * half, half, 1)
    bias = lax.dynamic_slice_in_dim(conv_b, odd * half, half, 0)
    sums = gate_up(
        *([slots[j] for j in range(4)] for slots in (own, other, edges)), w_gate, w_up, gu[:4]
    )
    act = activate_last(sums, gu[4:], taps, bias[None])

    away_other, away_own, here = down(act, w_down, dn)
    came = [send(away_other, "tp", xor_pairs(4, 1)), send(away_own, "tp", xor_pairs(4, 1))]

    middle = tokens // 16 * MIDDLE

    def partial(which, slot, rows):
        return here[which, slot, rows].astype(jnp.float32) + came[which][slot, rows].astype(jnp.float32)

    def cross(cells, axis, mask):
        return send(cells.astype(jnp.bfloat16), axis, xor_pairs(4, mask)).astype(jnp.float32)

    top, low = slice(0, middle), slice(middle, tokens)
    x_other = cross(partial(0, 1, top), "tp", 2)
    z_low = cross(jnp.stack([partial(0, 0, low), partial(0, 1, low)]), "sp", 1)
    x_top = cross(partial(1, 1, slice(0, middle + HALO)), "tp", 2)[:middle]
    back = cross(partial(0, 0, top) + x_other, "sp", 1)
    low_sum = (partial(1, 1, low) + z_low[1]).astype(jnp.bfloat16)
    x_low = cross(low_sum, "tp", 2)
    ffn = jnp.concatenate([partial(1, 0, top) + x_top + back, partial(1, 0, low) + z_low[0] + x_low])
    return (normed.astype(jnp.float32) + ffn).astype(jnp.bfloat16)


def solution(mesh):
    step = jax.shard_map(
        shards,
        mesh=mesh,
        in_specs=(
            P(("grp", "sp"), "tp"),
            P(("grp", "sp"), None),
            P(("grp", "sp"), None),
            P("tp"),
            P(("grp", "sp"), None),
            P(None, "tp"),
            P(),
            P("sp", "tp"),
            P("sp", "tp"),
            P(None, "tp"),
            P("tp"),
            P("tp", "sp"),
        ),
        out_specs=P(("grp", "sp"), "tp"),
        check_vma=False,
    )
    if not (mesh.shape["sp"] == mesh.shape["tp"] == 4 and mesh.shape["grp"] == 2):
        return step
    return step
```
